32 devices in a mesh: grp: 2 (over y), sp: 4 (over z), tp: 4 (over x, core).
Axes of the slice: x: 2, y: 2, z: 4, core: 2. Of those that a mesh axis runs over, the one named last changes fastest.
Arguments:
- tokens: bfloat16 [3072, 2048], P(('grp', 'sp'), 'tp'), parts along dimension 0, may hold values from -15 to 15
- gate_weight: bfloat16 [2, 2048, 2048], P(None, 'sp', 'tp'), may hold values from -0.125 to 0.125
- inner_weight: bfloat16 [2, 2048, 2048], P(None, 'sp', 'tp'), may hold values from -0.125 to 0.125
- value_weight: bfloat16 [2, 2048, 2048], P(None, 'sp', 'tp'), may hold values from -0.125 to 0.125
- out_weight: bfloat16 [2, 2048, 2048], P(None, 'tp', 'sp'), may hold values from -0.125 to 0.125
- taps: bfloat16 [2, 3, 2048], P(None, None, 'tp'), may hold values from -3 to 3
- norm_gain: float32 [2, 2048], P(None, 'tp'), may hold values from 0.1 to 1.9
- norm_bias: float32 [2, 2048], P(None, 'tp'), may hold values from -1.5 to 1.5
Outputs:
- mixed: bfloat16 [3072, 2048], P(('grp', 'sp'), 'tp'), parts along dimension 0
The draws below stay inside these ranges and needn't reach their ends.
There are 2 independent parts, one for each index of `grp`. The reference program is written for one: setup_inputs(seed, part) draws one part's arguments, and reference() takes and returns one part's arrays. A program takes and returns all parts, laid end to end along the dimension named above; an argument that names none is the same for every part. Nothing has to cross between parts.
All inputs are finite; a program needn't handle non-finite values.
Results may differ from the reference program's by a relative error of at most 0.03.
Values may be sent and summed in bfloat16 or wider, within the bound.
No kernel may reach another device: no remote copies, remote signals or barrier semaphores. Data moves between devices by JAX's collectives and lax.ppermute only.
A program may use at most 64 MiB of HBM per device.

```python
import jax
import jax.numpy as jnp
from jax import lax

D = 2048
LAYERS = 2
TOKENS = 1536
N_TP = 4


def draw_tokens(key, part):
    base_key = jax.random.fold_in(key, 11)
    scale_key = jax.random.fold_in(key, 12)
    base = jnp.clip(jax.random.normal(base_key, (TOKENS, D), jnp.float32), -6.0, 6.0)
    levels = jnp.exp(jax.random.uniform(scale_key, (D // 32,), jnp.float32, -0.9, 0.9))
    scales = jnp.repeat(levels, 32)
    return (base * scales[None, :]).astype(jnp.bfloat16)


def steps_of(key, shape, pieces, least, high):
    factor_of = 1.0
    for axis_at, shards_of in pieces:
        steps = jax.random.uniform(jax.random.fold_in(jax.random.fold_in(key, 6), axis_at), (shards_of,), jnp.float32, least / len(pieces), high / len(pieces))
        factor_of = factor_of * jnp.repeat(jnp.exp(steps), shape[axis_at] // shards_of).reshape((-1,) + (1,) * (len(shape) - 1 - axis_at))
    return factor_of


def scatter_about(own_key, dims, scale, most, split=(), kind=jnp.bfloat16):
    drawn = jax.random.normal(own_key, dims, jnp.float32) * scale
    if len(split) > 0:
        drawn = steps_of(own_key, dims, split, -0.22, 0.18) * drawn
    return jnp.clip(drawn, min=-most, max=most).astype(kind)


def setup_inputs(seed: int = 0, part: int = 0) -> dict:
    key_of = jax.random.split(jax.random.key(seed), 9)
    part_splits = jax.random.split(jax.random.fold_in(key_of[8], part), 9)
    return {
        "tokens": draw_tokens(jax.random.fold_in(jax.random.fold_in(key_of[8], part), 71), part),
        "gate_weight": scatter_about(key_of[1], (LAYERS, D, D), D ** -0.5, 0.125, ((1, 4), (2, 4))),
        "inner_weight": scatter_about(key_of[2], (LAYERS, D, D), D ** -0.5, 0.125, ((1, 4), (2, 4))),
        "value_weight": scatter_about(key_of[3], (LAYERS, D, D), D ** -0.5, 0.125, ((1, 4), (2, 4))),
        "out_weight": scatter_about(key_of[4], (LAYERS, D, D), D ** -0.5, 0.125, ((1, 4), (2, 4))),
        "taps": scatter_about(key_of[5], (LAYERS, 3, D), 0.6, 3.0, ((2, 4),)),
        "norm_gain": jnp.clip(1.0 + 0.18 * jax.random.normal(key_of[6], (LAYERS, D), jnp.float32), 0.1, 1.9),
        "norm_bias": scatter_about(key_of[7], (LAYERS, D), 0.3, 1.5, ((1, 4),), jnp.float32),
    }


def reference(tokens, gate_weight, inner_weight, value_weight, out_weight, taps, norm_gain, norm_bias):
    x = tokens
    block = D // N_TP
    for layer in range(LAYERS):
        outer = jnp.dot(x, gate_weight[layer], preferred_element_type=jnp.float32).astype(jnp.bfloat16)
        inner = jnp.dot(x, inner_weight[layer], preferred_element_type=jnp.float32).astype(jnp.bfloat16)
        values = jnp.dot(x, value_weight[layer], preferred_element_type=jnp.float32).astype(jnp.bfloat16)
        product = (inner.astype(jnp.float32) * values.astype(jnp.float32)).astype(jnp.bfloat16)
        padded = jnp.pad(product.astype(jnp.float32), ((1, 1), (0, 0)))
        kernel = taps[layer].astype(jnp.float32)
        conv = kernel[0] * padded[:-2] + kernel[1] * padded[1:-1] + kernel[2] * padded[2:]
        gated = (outer.astype(jnp.float32) * conv).astype(jnp.bfloat16)
        branch = jnp.zeros((x.shape[0], D), jnp.float32)
        for index in range(N_TP):
            part_rows = gated[:, index * block:(index + 1) * block]
            part_weight = out_weight[layer][index * block:(index + 1) * block, :]
            term = jnp.dot(part_rows, part_weight, preferred_element_type=jnp.float32).astype(jnp.bfloat16)
            branch = branch + term.astype(jnp.float32)
        total = 2.0 ** 0.5 * x.astype(jnp.float32) + branch
        mean = lax.optimization_barrier(jnp.sum(total, axis=1, keepdims=True)) / D
        square = lax.optimization_barrier(jnp.sum(total * total, axis=1, keepdims=True)) / D
        spread = square - mean * mean
        x = ((total - mean) * lax.rsqrt(spread + 1e-05) * norm_gain[layer] + norm_bias[layer]).astype(jnp.bfloat16)
    return x
```

```python
import jax
import jax.numpy as jnp
from jax import lax
from jax.sharding import PartitionSpec as P

CORES = 2


def shift(value, axis, by):
    peers = lax.axis_size(axis)
    return lax.ppermute(value, axis, [(i, (i + by) % peers) for i in range(peers)])


def core_shift(value, by):
    peers = lax.axis_size("tp")
    pairs = [(i, i - i % CORES + (i % CORES + by) % CORES) for i in range(peers)]
    return lax.ppermute(value, "tp", pairs)


def chip_shift(value, by):
    return shift(value, "tp", by * CORES)


def ring(own):
    groups, peers = lax.axis_size("grp"), lax.axis_size("sp")
    g = lax.axis_index("grp")
    pieces = [[own[(g + j) % groups] for j in range(groups)]]
    moving = pieces[0][0]
    for _ in range(1, peers):
        moving = shift(moving, "sp", 1)
        pieces.append([moving] + [shift(moving, "grp", groups - j) for j in range(1, groups)])
    return pieces


def gather_tp(x):
    chips = lax.axis_size("tp") // CORES
    columns = [x] + [chip_shift(x, b) for b in range(1, chips)]
    return [[c] + [core_shift(c, a) for a in range(1, CORES)] for c in columns]


def scatter_tp(blocks):
    chips = lax.axis_size("tp") // CORES
    sums = []
    for b in list(range(1, chips)) + [0]:
        part = blocks(b, 0).astype(jnp.float32)
        for a in range(1, CORES):
            part = part + core_shift(blocks(b, a), a).astype(jnp.float32)
        if b:
            part = chip_shift(part.astype(jnp.bfloat16), b).astype(jnp.float32)
        sums.append(part)
    total = sums[-1]
    for part in sums[:-1]:
        total = total + part
    return total


def shards(tokens, gate_weight, inner_weight, value_weight, out_weight, taps, norm_gain, norm_bias):
    layers = gate_weight.shape[0]
    groups, peers, ranks = lax.axis_size("grp"), lax.axis_size("sp"), lax.axis_size("tp")
    chips = ranks // CORES
    s, t, g = lax.axis_index("sp"), lax.axis_index("tp"), lax.axis_index("grp")
    chip, core = t // CORES, t % CORES
    rows, local = tokens.shape
    width = local * ranks
    block = gate_weight.shape[1]
    share = block // groups
    f32, bf16 = jnp.float32, jnp.bfloat16

    def dot(a, b):
        return jnp.dot(a, b, preferred_element_type=f32)

    rings = []
    for layer in range(layers):
        mixed = jnp.concatenate([inner_weight[layer], value_weight[layer]], axis=1)
        gate, out = gate_weight[layer], out_weight[layer]
        rings.append((
            ring(mixed.reshape(groups, share, -1)),
            ring(gate.reshape(groups, share, -1)),
            ring(out.reshape(groups, out.shape[0] // groups, -1)),
        ))

    x = tokens
    for layer in range(layers):
        mixed, gate, out = rings[layer]
        near = gather_tp(x)
        stacked = jnp.stack([near[b][a] for b in range(chips) for a in range(CORES)])
        whole = jnp.concatenate(
            [
                stacked[((chip - j // CORES) % chips) * CORES + (core - j % CORES) % CORES]
                for j in range(ranks)
            ],
            axis=1,
        )
        cut = jnp.stack([whole[:, i * share : (i + 1) * share] for i in range(width // share)])
        both, outer = 0.0, 0.0
        for k in range(peers):
            for j in range(groups):
                a = cut[((s - k) % peers) * groups + (g + j) % groups]
                both = both + dot(a, mixed[k][j])
                outer = outer + dot(a, gate[k][j])
        inner, values = both[:, :local].astype(bf16), both[:, local:].astype(bf16)
        outer = outer.astype(bf16)
        product = (inner.astype(f32) * values.astype(f32)).astype(bf16)
        up = [(i, i + 1) for i in range(peers - 1)]
        before = lax.ppermute(product[-1:], "sp", up)
        after = lax.ppermute(product[:1], "sp", [(j, i) for i, j in up])
        padded = jnp.concatenate([before, product, after], axis=0).astype(f32)
        kernel = taps[layer].astype(f32)
        conv = kernel[0] * padded[:-2] + kernel[1] * padded[1:-1] + kernel[2] * padded[2:]
        gated = (outer.astype(f32) * conv).astype(bf16)
        part = local // groups
        halves = jnp.stack([gated[:, i * part : (i + 1) * part] for i in range(groups)])
        terms = []
        for k in range(peers):
            acc = 0.0
            for j in range(groups):
                acc = acc + dot(halves[(g + j) % groups], out[k][j])
            terms.append(acc.astype(bf16))
        terms = jnp.stack(terms)
        ordered = jnp.concatenate([terms[(s - c) % peers] for c in range(peers)], axis=1)
        byrank = jnp.stack([ordered[:, j * local : (j + 1) * local] for j in range(ranks)])
        branch = scatter_tp(
            lambda b, a: byrank[((chip + b) % chips) * CORES + (core + a) % CORES]
        )
        total = 2.0**0.5 * x.astype(f32) + branch
        row_sum, row_square = lax.psum(
            (jnp.sum(total, axis=1), jnp.sum(total * total, axis=1)), "tp"
        )
        mean = (row_sum / width)[:, None]
        spread = (row_square / width)[:, None] - mean * mean
        x = (
            (total - mean) * lax.rsqrt(spread + 1e-05) * norm_gain[layer] + norm_bias[layer]
        ).astype(bf16)
    return x


def solution(mesh):
    in_specs = (
        P(("grp", "sp"), "tp"),
        P(None, "sp", "tp"),
        P(None, "sp", "tp"),
        P(None, "sp", "tp"),
        P(None, "tp", "sp"),
        P(None, None, "tp"),
        P(None, "tp"),
        P(None, "tp"),
    )
    out_specs = P(("grp", "sp"), "tp")
    return jax.shard_map(shards, mesh=mesh, in_specs=in_specs, out_specs=out_specs, check_vma=False)
```

```python
import jax
import jax.numpy as jnp
from jax import lax
from jax.sharding import PartitionSpec as P


CORES = 2


def shift(value, axis, by):
    peers = lax.axis_size(axis)
    return lax.ppermute(value, axis, [(i, (i + by) % peers) for i in range(peers)])


def core_shift(value, by):
    peers = lax.axis_size("tp")
    pairs = [(i, i - i % CORES + (i % CORES + by) % CORES) for i in range(peers)]
    return lax.ppermute(value, "tp", pairs)


def chip_shift(value, by):
    return shift(value, "tp", by * CORES)


def ring(own):
    groups, peers = lax.axis_size("grp"), lax.axis_size("sp")
    g = lax.axis_index("grp")
    pieces = [[own[(g + j) % groups] for j in range(groups)]]
    moving = pieces[0][0]
    for _ in range(1, peers):
        moving = shift(moving, "sp", 1)
        others = [shift(moving, "grp", groups - j) for j in range(1, groups)]
        pieces.append([moving] + others)
    return pieces


def gather_tp(x):
    chips = lax.axis_size("tp") // CORES
    columns = [x] + [chip_shift(x, b) for b in range(1, chips)]
    return [[c] + [core_shift(c, a) for a in range(1, CORES)] for c in columns]


def scatter_tp(blocks):
    chips = lax.axis_size("tp") // CORES
    sums = []
    for b in list(range(1, chips)) + [0]:
        part = blocks(b, 0).astype(jnp.float32)
        for a in range(1, CORES):
            part = part + core_shift(blocks(b, a), a).astype(jnp.float32)
        if b:
            part = chip_shift(part.astype(jnp.bfloat16), b).astype(jnp.float32)
        sums.append(part)
    total = sums[-1]
    for part in sums[:-1]:
        total = total + part
    return total


def shards(tokens, gate_weight, inner_weight, value_weight, out_weight, taps, norm_gain, norm_bias):
    layers = gate_weight.shape[0]
    groups, peers, ranks = lax.axis_size("grp"), lax.axis_size("sp"), lax.axis_size("tp")
    chips = ranks // CORES
    s, t, g = lax.axis_index("sp"), lax.axis_index("tp"), lax.axis_index("grp")
    chip, core = t // CORES, t % CORES
    _, local = tokens.shape
    width = local * ranks
    block = gate_weight.shape[1]
    share = block // groups
    f32, bf16 = jnp.float32, jnp.bfloat16

    def dot(a, b):
        return jnp.dot(a, b, preferred_element_type=f32)

    rings = []
    for layer in range(layers):
        mixed = jnp.concatenate([inner_weight[layer], value_weight[layer]], axis=1)
        gate, out = gate_weight[layer], out_weight[layer]
        rings.append((
            ring(mixed.reshape(groups, share, -1)),
            ring(gate.reshape(groups, share, -1)),
            ring(out.reshape(groups, out.shape[0] // groups, -1)),
        ))

    x = tokens
    for layer in range(layers):
        mixed, gate, out = rings[layer]
        near = gather_tp(x)
        stacked = jnp.stack([near[b][a] for b in range(chips) for a in range(CORES)])
        whole = jnp.concatenate(
            [
                stacked[((chip - j // CORES) % chips) * CORES + (core - j % CORES) % CORES]
                for j in range(ranks)
            ],
            axis=1,
        )
        cut = jnp.stack([whole[:, i * share : (i + 1) * share] for i in range(width // share)])
        both, outer = 0.0, 0.0
        for k in range(peers):
            for j in range(groups):
                a = cut[((s - k) % peers) * groups + (g + j) % groups]
                both = both + dot(a, mixed[k][j])
                outer = outer + dot(a, gate[k][j])
        inner, values = both[:, :local].astype(bf16), both[:, local:].astype(bf16)
        outer = outer.astype(bf16)
        product = (inner.astype(f32) * values.astype(f32)).astype(bf16)
        up = [(i, i + 1) for i in range(peers - 1)]
        before = lax.ppermute(product[-1:], "sp", up)
        after = lax.ppermute(product[:1], "sp", [(j, i) for i, j in up])
        padded = jnp.concatenate([before, product, after], axis=0).astype(f32)
        kernel = taps[layer].astype(f32)
        conv = kernel[0] * padded[:-2] + kernel[1] * padded[1:-1] + kernel[2] * padded[2:]
        gated = (outer.astype(f32) * conv).astype(bf16)
        part = local // groups
        halves = jnp.stack([gated[:, i * part : (i + 1) * part] for i in range(groups)])
        terms = []
        for k in range(peers):
            acc = 0.0
            for j in range(groups):
                acc = acc + dot(halves[(g + j) % groups], out[k][j])
            terms.append(acc.astype(bf16))
        terms = jnp.stack(terms)
        ordered = jnp.concatenate([terms[(s - c) % peers] for c in range(peers)], axis=1)
        byrank = jnp.stack([ordered[:, j * local : (j + 1) * local] for j in range(ranks)])
        branch = scatter_tp(lambda b, a: byrank[((chip + b) % chips) * CORES + (core + a) % CORES])
        total = 2.0**0.5 * x.astype(f32) + branch
        row_sum, row_square = lax.psum(
            (jnp.sum(total, axis=1), jnp.sum(total * total, axis=1)), "tp"
        )
        mean = (row_sum / width)[:, None]
        spread = (row_square / width)[:, None] - mean * mean
        x = (
            (total - mean) * lax.rsqrt(spread + 1e-05) * norm_gain[layer] + norm_bias[layer]
        ).astype(bf16)
    return x


def solution(mesh):
    in_specs = (
        P(("grp", "sp"), "tp"),
        P(None, "sp", "tp"),
        P(None, "sp", "tp"),
        P(None, "sp", "tp"),
        P(None, "tp", "sp"),
        P(None, None, "tp"),
        P(None, "tp"),
        P(None, "tp"),
    )
    out_specs = P(("grp", "sp"), "tp")

    step = jax.shard_map(shards, mesh=mesh, in_specs=in_specs, out_specs=out_specs, check_vma=False)
    return lambda *args: step(*args)
```
